128 devices in a mesh: sp: 32 (over z, y, core), tp: 4 (over x).
Axes of the slice: x: 4, y: 4, z: 4, core: 2. Of those that a mesh axis runs over, the one named last changes fastest.
Arguments:
- tokens: bfloat16 [1024, 48, 1024], P('sp', 'tp'), may hold values from -6 to 6
- norm_gain: float32 [1024], replicated, may hold values from 0.1 to 1.9
- x_weight: bfloat16 [1024, 1024], P(('sp', 'tp')), may hold values from -0.1875 to 0.1875
- gate_weight: bfloat16 [1024, 1024], P(('sp', 'tp')), may hold values from -0.1875 to 0.1875
- conv_taps: float32 [4, 1024], replicated, may hold values from -3 to 3
- rate_map: bfloat16 [2, 1024, 128], P(None, ('sp', 'tp')), may hold values from -0.5 to 0.5
- input_map: bfloat16 [2, 1024, 128], P(None, ('sp', 'tp')), may hold values from -0.5 to 0.5
- decay_rate: float32 [2, 1024], replicated, may hold values from 0.1 to 3
- out_weight: bfloat16 [1024, 1024], P(None, ('sp', 'tp')), may hold values from -0.5 to 0.5
Outputs:
- mixed_out: bfloat16 [1024, 48, 1024], P('sp', 'tp')
The draws below stay inside these ranges and needn't reach their ends.
All inputs are finite; a program needn't handle non-finite values.
Results may differ from the reference program's by a relative error of at most 0.004.
Values may be sent and summed in bfloat16 or wider, within the bound.
No kernel may reach another device: no remote copies, remote signals or barrier semaphores. Data moves between devices by JAX's collectives and lax.ppermute only.
A program may use at most 128 MiB of HBM per device.

```python
import math
import jax
import jax.numpy as jnp
from jax import lax

D = 1024
RNN_WIDTH = 1024
CONV_W = 4
SEQS = 48
RNN_BLOCK = 128
SEQ_LEN = 1024


def block_scale(key, extent, pieces, low, top_value):
    gain = 1.0
    for axis_at, blocks in pieces:
        draws = jax.random.uniform(jax.random.fold_in(jax.random.fold_in(key, 6), axis_at), (blocks,), jnp.float32, low / len(pieces), top_value / len(pieces))
        gain = gain * jnp.repeat(jnp.exp(draws), extent[axis_at] // blocks).reshape((-1,) + (1,) * (len(extent) - 1 - axis_at))
    return gain


def gaussian(rng, dims, width, most, cuts=(), dtype=jnp.bfloat16):
    factor_of = block_scale(rng, dims, cuts, -0.22, 0.18) if cuts else 1.0
    values = jax.random.normal(rng, dims, jnp.float32) * width * factor_of
    return jnp.minimum(jnp.maximum(values, -most), most).astype(dtype)


def setup_inputs(seed: int = 0) -> dict:
    key_list = jax.random.split(jax.random.key(seed), 10)
    return {
        "tokens": gaussian(key_list[0], (SEQ_LEN, SEQS, D), 1.0, 6.0, ((0, 32), (1, 4))),
        "norm_gain": jnp.clip(1.0 + 0.18 * jax.random.normal(key_list[1], (D,), jnp.float32), 0.1, 1.9),
        "x_weight": gaussian(key_list[2], (D, RNN_WIDTH), D ** -0.5, 0.1875, ((0, 128),)),
        "gate_weight": gaussian(key_list[3], (D, RNN_WIDTH), D ** -0.5, 0.1875, ((0, 128),)),
        "conv_taps": gaussian(key_list[4], (CONV_W, RNN_WIDTH), CONV_W ** -0.5, 3.0, (), jnp.float32),
        "rate_map": gaussian(key_list[5], (2, RNN_WIDTH, RNN_BLOCK), RNN_BLOCK ** -0.5, 0.5, ((1, 128),)),
        "input_map": gaussian(key_list[6], (2, RNN_WIDTH, RNN_BLOCK), RNN_BLOCK ** -0.5, 0.5, ((1, 128),)),
        "decay_rate": jnp.clip(jnp.exp(jax.random.uniform(key_list[7], (2, RNN_WIDTH), jnp.float32, math.log(0.1), math.log(3.0))), 0.1, 3.0),
        "out_weight": gaussian(key_list[8], (RNN_WIDTH, D), (RNN_WIDTH // 8) ** -0.5, 0.5, ((1, 128),)),
    }


epsilon = 1e-06

def recur(conv_block, rate_block, input_block, speed, reverse):
    conv_f = conv_block.astype(jnp.float32)
    rate_gate = jax.nn.sigmoid(jnp.einsum('tsc,cd->tsd', conv_f, rate_block.astype(jnp.float32)))
    input_gate = jax.nn.sigmoid(jnp.einsum('tsc,cd->tsd', conv_f, input_block.astype(jnp.float32)))
    log_decay = -2.0 * rate_gate * speed / SEQ_LEN
    decay = jnp.exp(log_decay)
    drive = jnp.sqrt(-jnp.expm1(2.0 * log_decay)) * input_gate * conv_f

    def advance(state, inputs):
        step_decay, step_drive = inputs
        state = step_decay * state + step_drive
        return (state, state)
    initial = jnp.zeros(conv_block.shape[1:], jnp.float32)
    _, states = lax.scan(advance, initial, (decay, drive), reverse=reverse)
    return states

def reference(tokens, norm_gain, x_weight, gate_weight, conv_taps, rate_map, input_map, decay_rate, out_weight):
    length, seqs, width_in = tokens.shape
    flt = tokens.astype(jnp.float32)
    scale = lax.rsqrt(lax.optimization_barrier(jnp.mean(flt * flt, axis=-1, keepdims=True)) + epsilon)
    normed = (flt * scale * norm_gain).astype(jnp.bfloat16)
    flat = normed.reshape(length * seqs, width_in)
    channels = x_weight.shape[1]
    branch = jnp.dot(flat, x_weight, preferred_element_type=jnp.float32).astype(jnp.bfloat16).reshape(length, seqs, channels)
    gate_in = jnp.dot(flat, gate_weight, preferred_element_type=jnp.float32).astype(jnp.bfloat16).reshape(length, seqs, channels)
    padded = jnp.pad(branch, ((2, 1), (0, 0), (0, 0))).astype(jnp.float32)
    conv = padded[0:length] * conv_taps[0]
    for offset in range(1, 4):
        conv = conv + padded[offset:offset + length] * conv_taps[offset]
    conv_bf = lax.optimization_barrier(conv.astype(jnp.bfloat16))
    block_width = rate_map.shape[2]
    nblk = channels // block_width
    rate_blocks = rate_map.reshape(2, nblk, block_width, block_width)
    input_blocks = input_map.reshape(2, nblk, block_width, block_width)
    blocked = conv_bf.reshape(length, seqs, nblk, -1).transpose(2, 0, 1, 3)

    def per_block(inputs):
        conv_block, rate_fwd, rate_bwd, input_fwd, input_bwd, speed_fwd, speed_bwd = inputs
        forward = recur(conv_block, rate_fwd, input_fwd, speed_fwd, False)
        backward = recur(conv_block, rate_bwd, input_bwd, speed_bwd, True)
        return (forward + backward).astype(jnp.bfloat16)
    recurrent = lax.map(per_block, (blocked, rate_blocks[0], rate_blocks[1], input_blocks[0], input_blocks[1], decay_rate[0].reshape(nblk, -1), decay_rate[1].reshape(nblk, -1)))
    recurrent = recurrent.transpose(1, 2, 0, 3).reshape(length, seqs, channels)
    recurrent = lax.optimization_barrier(recurrent)
    gated = (recurrent.astype(jnp.float32) * jax.nn.gelu(gate_in.astype(jnp.float32))).astype(jnp.bfloat16)
    result = jnp.dot(gated.reshape(length * seqs, channels), out_weight, preferred_element_type=jnp.float32)
    return result.astype(jnp.bfloat16).reshape(length, seqs, width_in)
```

```python
import jax
import jax.numpy as jnp
from jax import lax
from jax.experimental import pallas as pl
from jax.experimental.pallas import tpu as pltpu
from jax.sharding import Mesh
from jax.sharding import PartitionSpec as P

F32 = jnp.float32
BF16 = jnp.bfloat16
ALL = ("z", "y", "c", "x")
SP = ("z", "y", "c")
EPS = 1e-06
STEPS = 8
CHAINS = 48
ROWS = STEPS * CHAINS
HALO = 3 * CHAINS
LANES = 128
WIDE = 256


def flat_index(z, y, c, x):
    return ((z * 4 + y) * 2 + c) * 4 + x


def shift_pairs(axis, amount, mirrored=False):
    pairs = []
    for z in range(4):
        for y in range(4):
            for c in range(2):
                for x in range(4):
                    at = {"z": z, "y": y, "c": c, "x": x}
                    to = dict(at)
                    if axis == "c":
                        to["c"] = 1 - c
                    else:
                        step = -amount if (mirrored and c == 1) else amount
                        to[axis] = (at[axis] + step) % 4
                    pairs.append((flat_index(**at), flat_index(**to)))
    return pairs


BIT_DIM = {
    ("z", 1): 0,
    ("z", 0): 1,
    ("y", 1): 2,
    ("y", 0): 3,
    ("c", 0): 4,
    ("x", 1): 5,
    ("x", 0): 6,
}


def doubled(block, axis, bit):
    if axis == "c":
        mine = lax.axis_index("c")
        pairs = shift_pairs("c", 1)
    else:
        mine = (lax.axis_index(axis) >> bit) & 1
        pairs = shift_pairs(axis, 2 if bit else 1, mirrored=True)
    other = lax.ppermute(block, ALL, pairs)
    low = jnp.where(mine == 1, other, block)
    high = jnp.where(mine == 1, block, other)
    return jnp.concatenate([low, high], axis=BIT_DIM[(axis, bit)])


def gathered(parts, orders):
    blocks = [p.reshape((1,) * 7 + p.shape) for p in parts]
    for bit in (1, 0):
        for k in range(3):
            blocks = [doubled(b, order[k], bit) for b, order in zip(blocks, orders)]
    blocks = [doubled(b, "c", 0) for b in blocks]
    return [b.reshape(1024, b.shape[-1]) for b in blocks]


def norm_kernel(tok_ref, halo_ref, gain_ref, out_ref, scratch):
    gain = gain_ref[...]

    def normed(rows):
        flt = rows.astype(F32)
        mean = jnp.mean(flt * flt, axis=-1, keepdims=True)
        return flt * lax.rsqrt(mean + EPS) * gain

    for start in range(0, ROWS, 64):
        part = normed(tok_ref[start : start + 64, :])
        for b in range(8):
            scratch[b, start : start + 64, :] = part[:, b * LANES : (b + 1) * LANES]
    for t in range(STEPS):
        for b in range(8):
            rows = scratch[b, pl.ds(t, CHAINS, stride=STEPS), :]
            out_ref[t * CHAINS : (t + 1) * CHAINS, b * LANES : (b + 1) * LANES] = rows.astype(BF16)
    for k in range(3):
        part = normed(halo_ref[k])
        out_ref[ROWS + k * CHAINS : ROWS + (k + 1) * CHAINS, :] = part.astype(BF16)


def local_kernel(
    normed_ref, xw_ref, rate0_ref, rate1_ref, in0_ref, in1_ref, taps_ref, speed_ref,
    hsum_ref, pf_ref, pb_ref, ends_ref, total_ref,
):
    branch = jnp.dot(normed_ref[...], xw_ref[...], preferred_element_type=F32)
    branch = branch.astype(BF16).astype(F32)
    place = lax.broadcasted_iota(jnp.int32, (CHAINS, LANES), 0) & 3
    first, last = place == 0, place == 3
    for half in range(WIDE // LANES):
        cols = slice(half * LANES, (half + 1) * LANES)
        rows = [branch[t * CHAINS : (t + 1) * CHAINS, cols] for t in range(STEPS + 3)]
        step = rows[:STEPS]
        before2, before1, after1 = rows[STEPS:]
        wrap6 = jnp.where(first, before2, pltpu.roll(step[6], 1, 0))
        wrap7 = jnp.where(first, before1, pltpu.roll(step[7], 1, 0))
        wrap0 = jnp.where(last, after1, pltpu.roll(step[0], CHAINS - 1, 0))
        line = [wrap6, wrap7] + step + [wrap0]
        taps = [taps_ref[j : j + 1, cols] for j in range(4)]
        conv = []
        for t in range(STEPS):
            acc = line[t] * taps[0]
            for j in range(1, 4):
                acc = acc + line[t + j] * taps[j]
            conv.append(acc.astype(BF16))
        halves = [(c.astype(F32) * 0.5) for c in conv]
        stacked = jnp.concatenate([h.astype(BF16) for h in halves], axis=0)
        mrows = slice(half * LANES, (half + 1) * LANES)
        for k, (rate_ref, in_ref) in enumerate(((rate0_ref, in0_ref), (rate1_ref, in1_ref))):
            rate = jnp.dot(stacked, rate_ref[mrows, :], preferred_element_type=F32)
            gate = jnp.dot(stacked, in_ref[mrows, :], preferred_element_type=F32)
            speed = speed_ref[k : k + 1, cols] * (1.0 / 1024.0)
            order = range(STEPS) if k == 0 else range(STEPS - 1, -1, -1)
            state = prod = None
            for t in order:
                span = slice(t * CHAINS, (t + 1) * CHAINS)
                rise = speed * jnp.tanh(rate[span]) + speed
                lost = rise * (1.0 - rise * (0.5 - rise * (1.0 / 6.0 - rise * (1.0 / 24.0))))
                decay = 1.0 - lost
                square = lost * (1.0 + decay)
                root = square * lax.rsqrt(jnp.maximum(square, 1e-37))
                drive = root * (halves[t] * jnp.tanh(gate[span]) + halves[t])
                if state is None:
                    state, prod = drive, decay
                else:
                    state, prod = decay * state + drive, prod * decay
                if k == 0:
                    hsum_ref[span, cols] = state
                    pf_ref[span, cols] = prod
                else:
                    hsum_ref[span, cols] = hsum_ref[span, cols] + state
                    pb_ref[span, cols] = prod
            ends_ref[2 * k, half] = prod
            ends_ref[2 * k + 1, half] = state
            pieces = range(4) if k == 0 else range(3, -1, -1)
            ta = tb = None
            for q in pieces:
                qa = ends_ref[2 * k, half, pl.ds(q, 12, stride=4), :]
                qb = ends_ref[2 * k + 1, half, pl.ds(q, 12, stride=4), :]
                ta, tb = (qa, qb) if ta is None else (qa * ta, qa * tb + qb)
            total_ref[2 * k, :, cols] = ta
            total_ref[2 * k + 1, :, cols] = tb


def gate_kernel(normed_ref, gw_ref, out_ref):
    gate_in = jnp.dot(normed_ref[...], gw_ref[...], preferred_element_type=F32)
    out_ref[...] = jax.nn.gelu(gate_in.astype(BF16).astype(F32))


def out_kernel(
    hsum_ref, pf_ref, pb_ref, ends_ref, carry_ref, gelu_ref, ow_ref, out_ref, gated, chains, rows
):
    for half in range(WIDE // LANES):
        cols = slice(half * LANES, (half + 1) * LANES)
        for k in range(2):
            value = carry_ref[k, :, cols]
            pieces = range(4) if k == 0 else range(3, -1, -1)
            for n, q in enumerate(pieces):
                chains[k, pl.ds(q, 12, stride=4), :] = value
                if n < 3:
                    qa = ends_ref[2 * k, half, pl.ds(q, 12, stride=4), :]
                    qb = ends_ref[2 * k + 1, half, pl.ds(q, 12, stride=4), :]
                    value = qa * value + qb
        inf, inb = chains[0], chains[1]
        block = pl.program_id(0) * 2 + half
        for t in range(STEPS):
            span = slice(t * CHAINS, (t + 1) * CHAINS)
            both = hsum_ref[span, cols] + pf_ref[span, cols] * inf + pb_ref[span, cols] * inb
            recurrent = both.astype(BF16).astype(F32)
            gated[block, span, :] = (recurrent * gelu_ref[span, cols]).astype(BF16)

    @pl.when(pl.program_id(0) == pl.num_programs(0) - 1)
    def _():
        left = jnp.concatenate([gated[b] for b in range(8)], axis=1)
        for n in range(4):
            out = lax.dot_general(
                left,
                ow_ref[n * 256 : (n + 1) * 256, :],
                (((1,), (1,)), ((), ())),
                preferred_element_type=F32,
            )
            for half in range(2):
                for t in range(STEPS):
                    rows[pl.ds(t, CHAINS, stride=STEPS), :] = out[
                        t * CHAINS : (t + 1) * CHAINS, half * LANES : (half + 1) * LANES
                    ]
                at = n * 256 + half * LANES
                out_ref[:, at : at + LANES] = rows[...].astype(BF16)


def params(semantics):
    return pltpu.CompilerParams(dimension_semantics=semantics)


def run_norm(tok, halo, gain):
    return pl.pallas_call(
        norm_kernel,
        out_shape=jax.ShapeDtypeStruct((ROWS + HALO, 1024), BF16),
        scratch_shapes=[pltpu.VMEM((8, ROWS, LANES), F32)],
        name="norm",
    )(tok, halo, gain)


def run_local(normed, w0, w1, w2, taps, speed):
    full = ROWS + HALO
    wide = pl.BlockSpec((ROWS, WIDE), lambda b: (0, b))
    return pl.pallas_call(
        local_kernel,
        grid=(1024 // WIDE,),
        in_specs=[
            pl.BlockSpec((full, 1024), lambda b: (0, 0)),
            pl.BlockSpec((1024, WIDE), lambda b: (0, b)),
            pl.BlockSpec((WIDE, LANES), lambda b: (b, 8)),
            pl.BlockSpec((WIDE, LANES), lambda b: (b, 9)),
            pl.BlockSpec((WIDE, LANES), lambda b: (b, 8)),
            pl.BlockSpec((WIDE, LANES), lambda b: (b, 8)),
            pl.BlockSpec((4, WIDE), lambda b: (0, b)),
            pl.BlockSpec((2, WIDE), lambda b: (0, b)),
        ],
        out_specs=[
            wide,
            wide,
            wide,
            pl.BlockSpec((4, WIDE // LANES, CHAINS, LANES), lambda b: (0, b, 0, 0)),
            pl.BlockSpec((4, 12, WIDE), lambda b: (0, 0, b)),
        ],
        out_shape=[
            jax.ShapeDtypeStruct((ROWS, 1024), F32),
            jax.ShapeDtypeStruct((ROWS, 1024), F32),
            jax.ShapeDtypeStruct((ROWS, 1024), F32),
            jax.ShapeDtypeStruct((4, 8, CHAINS, LANES), F32),
            jax.ShapeDtypeStruct((4, 12, 1024), F32),
        ],
        compiler_params=params(("arbitrary",)),
        cost_estimate=pl.CostEstimate(flops=3_000_000_000, transcendentals=3_000_000, bytes_accessed=9_000_000),
        name="local",
    )(normed, w0, w0, w0, w1, w2, taps, speed)


def run_gate(normed, w1):
    return pl.pallas_call(
        gate_kernel,
        grid=(1024 // WIDE,),
        in_specs=[
            pl.BlockSpec((ROWS, 1024), lambda b: (0, 0)),
            pl.BlockSpec((1024, WIDE), lambda b: (0, b)),
        ],
        out_specs=pl.BlockSpec((ROWS, WIDE), lambda b: (0, b)),
        out_shape=jax.ShapeDtypeStruct((ROWS, 1024), F32),
        compiler_params=params(("arbitrary",)),
        cost_estimate=pl.CostEstimate(flops=1_000_000_000, transcendentals=400_000, bytes_accessed=4_500_000),
        name="gate",
    )(normed, w1)


def run_out(hsum, pf, pb, ends, carry, gelu, w2):
    wide = pl.BlockSpec((ROWS, WIDE), lambda b: (0, b))
    return pl.pallas_call(
        out_kernel,
        grid=(1024 // WIDE,),
        in_specs=[
            wide,
            wide,
            wide,
            pl.BlockSpec((4, WIDE // LANES, CHAINS, LANES), lambda b: (0, b, 0, 0)),
            pl.BlockSpec((2, 12, WIDE), lambda b: (0, 0, b)),
            wide,
            pl.BlockSpec((1024, 1024), lambda b: (0, 0)),
        ],
        out_specs=pl.BlockSpec((ROWS, 1024), lambda b: (0, 0)),
        out_shape=jax.ShapeDtypeStruct((ROWS, 1024), BF16),
        scratch_shapes=[
            pltpu.VMEM((8, ROWS, LANES), BF16),
            pltpu.VMEM((2, CHAINS, LANES), F32),
            pltpu.VMEM((ROWS, LANES), F32),
        ],
        compiler_params=params(("arbitrary",)),
        cost_estimate=pl.CostEstimate(flops=1_000_000_000, transcendentals=0, bytes_accessed=9_000_000),
        name="out",
    )(hsum, pf, pb, ends, carry, gelu, w2)


def after(earlier, later):
    return (earlier[0] * later[0], later[0] * earlier[1] + later[1])


def chosen(flag, pair, other):
    return tuple(jnp.where(flag, p, o) for p, o in zip(pair, other))


def packed_pair(forward, backward):
    return jnp.stack([jnp.log(forward[0]), forward[1], jnp.log(backward[0]), backward[1]]).astype(BF16)


def unpacked_pair(packed):
    wide = packed.astype(F32)
    return (jnp.exp(wide[0]), wide[1]), (jnp.exp(wide[2]), wide[3])


def carries(total):
    none = (jnp.ones_like(total[0]), jnp.zeros_like(total[0]))
    forward, backward = (total[0], total[1]), (total[2], total[3])
    core = lax.axis_index("c")
    other = lax.ppermute(total, "c", [(0, 1), (1, 0)])
    low = jnp.where(core == 0, total, other)
    high = jnp.where(core == 0, other, total)
    before_f = chosen(core == 1, (low[0], low[1]), none)
    before_b = chosen(core == 0, (high[2], high[3]), none)
    forward = after((low[0], low[1]), (high[0], high[1]))
    backward = after((high[2], high[3]), (low[2], low[3]))
    for axis in ("y", "z"):
        mine = lax.axis_index(axis)
        sent = packed_pair(forward, backward)
        got = {
            k: lax.ppermute(sent, axis, [(i, (i + k) % 4) for i in range(4)]) for k in (1, 3, 2)
        }
        parts = {k: unpacked_pair(v) for k, v in got.items()}
        ahead_f, ahead_b = none, none
        for k in (3, 2, 1):
            ahead_f = chosen(mine >= k, after(ahead_f, parts[k][0]), ahead_f)
        for k in (1, 2, 3):
            ahead_b = chosen(mine < k, after(ahead_b, parts[k][1]), ahead_b)
        if axis == "y":
            whole_f = after(ahead_f, forward)
            whole_b = after(ahead_b, backward)
            for k in (3, 2, 1):
                whole_f = chosen(mine < k, after(whole_f, parts[k][0]), whole_f)
            for k in (1, 2, 3):
                whole_b = chosen(mine >= k, after(whole_b, parts[k][1]), whole_b)
            forward, backward = whole_f, whole_b
        before_f = after(ahead_f, before_f)
        before_b = after(ahead_b, before_b)
    return jnp.stack([before_f[1], before_b[1]])


def repeated(rows):
    return jnp.broadcast_to(rows[:, None, :], (12, 4, 1024)).reshape(CHAINS, 1024)


def shards(
    tokens, norm_gain, x_weight, gate_weight, conv_taps, rate_map, input_map, decay_rate, out_weight
):
    out_rows = out_weight.T
    parts = [
        jnp.concatenate([x_weight, rate_map[0], rate_map[1]], axis=1),
        jnp.concatenate([gate_weight, input_map[0]], axis=1),
        jnp.concatenate([out_rows, input_map[1]], axis=1),
    ]
    tok = tokens.transpose(1, 0, 2)
    places = 32
    prev = lax.ppermute(tok[:, 30:32, :], SP, [(i, i + 1) for i in range(places - 1)])
    nxt = lax.ppermute(tok[:, 0:1, :], SP, [(i + 1, i) for i in range(places - 1)])
    halo = jnp.stack([repeated(prev[:, 0]), repeated(prev[:, 1]), repeated(nxt[:, 0])])
    normed = run_norm(tok.reshape(ROWS, 1024), halo, norm_gain.reshape(1, 1024))
    w0, w1, w2 = gathered(parts, [("x", "y", "z"), ("y", "z", "x"), ("z", "x", "y")])
    hsum, pf, pb, ends, total = run_local(normed, w0, w1, w2, conv_taps, decay_rate)
    gelu = run_gate(normed, w1)
    carry = carries(total)
    out = run_out(hsum, pf, pb, ends, carry, gelu, w2)
    return out.reshape(12, 32, 1024).transpose(1, 0, 2)


def solution(mesh):
    split = Mesh(mesh.devices.reshape(4, 4, 2, mesh.shape["tp"]), ALL)
    return jax.shard_map(
        shards,
        mesh=split,
        in_specs=(
            P(SP, "x", None),
            P(),
            P(ALL, None),
            P(ALL, None),
            P(),
            P(None, ALL, None),
            P(None, ALL, None),
            P(),
            P(None, ALL),
        ),
        out_specs=P(SP, "x", None),
        check_vma=False,
    )
```
